32 devices in a mesh: sp: 8 (over z, x), tp: 4 (over y, core).
Axes of the slice: x: 2, y: 2, z: 4, core: 2. Of those that a mesh axis runs over, the one named last changes fastest.
Arguments:
- tokens_in: bfloat16 [6144, 2048], P(('sp', 'tp')), may hold values from -300 to 300
- norm_gain: float32 [2048], replicated, may hold values from 0.1 to 1.9
- query_weight: bfloat16 [2048, 1024], P('sp', 'tp'), may hold values from -64 to 64
- key_weight: bfloat16 [2048, 512], P('sp', 'tp'), may hold values from -1 to 1
- value_weight: bfloat16 [2048, 512], P('sp', 'tp'), may hold values from -0.125 to 0.125
- pool_weight: bfloat16 [2048, 1024], P('sp', 'tp'), may hold values from -0.125 to 0.125
- sink_logit: float32 [16], P('tp'), may hold values from 1 to 5
- pool_gain: float32 [1024], P('tp'), may hold values from 0.1 to 1.9
- attention_out_weight: bfloat16 [1024, 2048], P('tp', 'sp'), may hold values from -0.125 to 0.125
- pool_out_weight: bfloat16 [1024, 2048], P('tp', 'sp'), may hold values from -0.1875 to 0.1875
Outputs:
- mixed_out: bfloat16 [6144, 2048], P(('sp', 'tp'))
The draws below stay inside these ranges and needn't reach their ends.
All inputs are finite; a program needn't handle non-finite values.
Results may differ from the reference program's by a relative error of at most 0.014.
Values may be sent and summed in bfloat16 or wider, within the bound.
No kernel may reach another device: no remote copies, remote signals or barrier semaphores. Data moves between devices by JAX's collectives and lax.ppermute only.
A program may use at most 64 MiB of HBM per device.

```python
import jax
import jax.numpy as jnp
from jax import lax

D = 2048
HEADS = 16
KV_HEADS = 8
HEAD_DIM = 64
POOL_CH = 256
POOL_GROUPS = 4
WINDOW = 128
TOK_DEV = 768
TOKENS = 6144
Q_WIDTH = 1024
KV_WIDTH = 512
POOL_WIDTH = 1024
N_TP = 4


def draw_tokens_in(key, part):
    noise_key = jax.random.fold_in(key, 11)
    direction_key = jax.random.fold_in(key, 12)
    level_key = jax.random.fold_in(key, 13)
    rough = jax.random.normal(noise_key, (TOKENS, D), jnp.float32)
    direction = jax.random.normal(direction_key, (D,), jnp.float32)
    block_count = TOKENS // TOK_DEV
    block_number = jnp.arange(block_count)
    ramp = block_number.astype(jnp.float32) / max(block_count - 1, 1)
    alternate = (1 - 2 * (block_number % 2)).astype(jnp.float32)
    jitter = jax.random.uniform(level_key, (block_count,), jnp.float32, 0.8, 1.3)
    levels = 2.0 * 3.0 ** ramp * jitter * alternate
    level_rows = jnp.repeat(levels, TOK_DEV)
    values = rough + level_rows[:, None] * direction[None, :]
    return jnp.clip(values, -300.0, 300.0).astype(jnp.bfloat16)


def key_base(key):
    limit = 6.0 * D ** (-0.5)
    base = jax.random.normal(jax.random.fold_in(key, 71), (D, KV_HEADS * HEAD_DIM), jnp.float32) * D ** (-0.5)
    base = jnp.clip(base, -limit, limit)
    return base


def draw_key_weight(key, part):
    return jnp.clip(key_base(key), -1.0, 1.0).astype(jnp.bfloat16)


def draw_query_weight(key, part):
    limit = 6.0 * D ** (-0.5)
    own = jax.random.normal(jax.random.fold_in(key, 72), (D, HEADS * HEAD_DIM), jnp.float32) * D ** (-0.5)
    own = jnp.clip(own, -limit, limit)
    return jnp.clip(own, -64.0, 64.0).astype(jnp.bfloat16)


def with_spikes(values, key, source, target, blocks, factor):
    owner, partner = [(jnp.arange(values.shape[dim]) // (values.shape[dim] // blocks)).reshape([-1 if axis == dim else 1 for axis in range(values.ndim)]) for dim in (source, target)]
    chosen = jax.random.permutation(key, blocks)[partner]
    strong = (owner == chosen) | (owner == (partner + blocks // 2) % blocks)
    return jnp.where(strong, factor * values, values)


def level_of(key, shape, split, low, largest):
    level = 1.0
    for dim, shards_of in split:
        steps = jax.random.uniform(jax.random.fold_in(jax.random.fold_in(key, 6), dim), (shards_of,), jnp.float32, low / len(split), largest / len(split))
        level = level * jnp.repeat(jnp.exp(steps), shape[dim] // shards_of).reshape((-1,) + (1,) * (len(shape) - 1 - dim))
    return level


def bell_draw(stream_key, dims, deviation, most, pieces=(), held_as=jnp.bfloat16):
    drawn = deviation * jax.random.normal(stream_key, dims, jnp.float32)
    if pieces:
        drawn = drawn * level_of(stream_key, dims, pieces, -0.22, 0.18)
    return jnp.clip(drawn, -most, most).astype(held_as)


def bell_draw_with(rng, dims, deviation, bound, shards, heavy, dtype=jnp.bfloat16):
    drawn = deviation * jax.random.normal(rng, dims, jnp.float32)
    if shards:
        drawn = drawn * level_of(rng, dims, shards, -0.22, 0.18)
    return jnp.clip(with_spikes(drawn, jax.random.fold_in(rng, 3), *heavy), -bound, bound).astype(dtype)


def setup_inputs(seed: int = 0) -> dict:
    keys = jax.random.split(jax.random.key(seed), 11)
    return {
        "tokens_in": draw_tokens_in(jax.random.fold_in(keys[10], 71), 0),
        "norm_gain": jnp.clip(1.0 + 0.18 * jax.random.normal(keys[1], (D,), jnp.float32), 0.1, 1.9),
        "query_weight": draw_query_weight(jax.random.fold_in(keys[10], 71), 0),
        "key_weight": draw_key_weight(jax.random.fold_in(keys[10], 71), 0),
        "value_weight": bell_draw(keys[4], (D, KV_WIDTH), D ** -0.5, 0.125, ((0, 8), (1, 4))),
        "pool_weight": bell_draw(keys[5], (D, POOL_WIDTH), D ** -0.5, 0.125, ((0, 8), (1, 4))),
        "sink_logit": jnp.clip(1.0 + 4.0 * jax.random.uniform(keys[6], (HEADS,), jnp.float32) ** level_of(keys[6], (HEADS,), ((0, 4),), -0.2, 0.2), 1.0, 5.0),
        "pool_gain": jnp.clip(1.0 + 0.18 * jax.random.normal(keys[7], (POOL_WIDTH,), jnp.float32), 0.1, 1.9),
        "attention_out_weight": bell_draw(keys[8], (Q_WIDTH, D), (Q_WIDTH + POOL_WIDTH) ** -0.5, 0.125, ((0, 4), (1, 8))),
        "pool_out_weight": bell_draw_with(keys[9], (POOL_WIDTH, D), (Q_WIDTH + POOL_WIDTH) ** -0.5, 0.1875, ((0, 4), (1, 8)), (0, 1, 8, 2.0)),
    }


EPS = 1e-06
SHORT_REACHES = (8, 32)

def attention_mix(query_rows, key_rows, value_rows, sink_logit):
    total_rows = query_rows.shape[0]
    blocks = total_rows // WINDOW
    group = HEADS // KV_HEADS
    queries = query_rows.astype(jnp.float32).reshape(blocks, WINDOW, KV_HEADS, group, HEAD_DIM)
    key_blocks = key_rows.astype(jnp.float32).reshape(blocks, WINDOW, KV_HEADS, HEAD_DIM)
    value_blocks = value_rows.astype(jnp.float32).reshape(blocks, WINDOW, KV_HEADS, HEAD_DIM)

    def with_previous(blocks_in):
        earlier = jnp.concatenate([jnp.zeros_like(blocks_in[:1]), blocks_in[:-1]], axis=0)
        return jnp.concatenate([earlier, blocks_in], axis=1)
    key_pairs = with_previous(key_blocks)
    value_pairs = with_previous(value_blocks)
    scores = jnp.einsum('nqhgd,nkhd->nhgqk', queries, key_pairs) * HEAD_DIM ** (-0.5)
    q_index = jnp.arange(WINDOW)[:, None]
    k_index = jnp.arange(2 * WINDOW)[None, :]
    distance = q_index + WINDOW - k_index
    inside = (distance >= 0) & (distance < WINDOW)
    block_index = jnp.arange(blocks)[:, None, None]
    allowed = inside[None] & ((block_index > 0) | (k_index >= WINDOW)[None])
    scores = jnp.where(allowed[:, None, None], scores, -jnp.inf)
    sinks = sink_logit.astype(jnp.float32).reshape(1, KV_HEADS, group, 1, 1)
    peak = jnp.maximum(lax.optimization_barrier(jnp.max(scores, axis=-1, keepdims=True)), sinks)
    expo = jnp.exp(scores - peak)
    denom = lax.optimization_barrier(jnp.sum(expo, axis=-1, keepdims=True)) + jnp.exp(sinks - peak)
    probs = lax.optimization_barrier((expo / denom).astype(jnp.bfloat16))
    attended = jnp.einsum('nhgqk,nkhd->nqhgd', probs.astype(jnp.float32), value_pairs)
    return attended.astype(jnp.bfloat16).reshape(total_rows, HEADS * HEAD_DIM)

def pool_mix(pool_rows, pool_gain):
    total_rows = pool_rows.shape[0]
    values = pool_rows.astype(jnp.float32)
    running = jnp.concatenate([jnp.zeros((1, values.shape[1]), jnp.float32), jnp.cumsum(values, axis=0)], axis=0)
    position = jnp.arange(total_rows)
    outputs = []
    for group_index, reach in enumerate(SHORT_REACHES + (WINDOW,)):
        span = running[:, group_index * POOL_CH:(group_index + 1) * POOL_CH]
        lower = span[jnp.maximum(position + 1 - reach, 0)]
        count = jnp.minimum(position + 1, reach).astype(jnp.float32)[:, None]
        outputs.append((span[1:] - lower) / count)
    whole_prefix = running[1:, (POOL_GROUPS - 1) * POOL_CH:] / (position + 1).astype(jnp.float32)[:, None]
    pooled = jnp.concatenate(outputs + [whole_prefix], axis=1)
    return ((pooled - values) * pool_gain.astype(jnp.float32)).astype(jnp.bfloat16)

def reference(tokens_in, norm_gain, query_weight, key_weight, value_weight, pool_weight, sink_logit, pool_gain, attention_out_weight, pool_out_weight):
    widened = tokens_in.astype(jnp.float32)
    inverse = lax.rsqrt(lax.optimization_barrier(jnp.mean(widened * widened, axis=1, keepdims=True)) + EPS)
    normed = (widened * inverse * norm_gain.astype(jnp.float32)).astype(jnp.bfloat16)
    query_rows = jnp.dot(normed, query_weight, preferred_element_type=jnp.float32).astype(jnp.bfloat16)
    key_rows = jnp.dot(normed, key_weight, preferred_element_type=jnp.float32).astype(jnp.bfloat16)
    value_rows = jnp.dot(normed, value_weight, preferred_element_type=jnp.float32).astype(jnp.bfloat16)
    pool_rows = jnp.dot(normed, pool_weight, preferred_element_type=jnp.float32).astype(jnp.bfloat16)
    attended = attention_mix(query_rows, key_rows, value_rows, sink_logit)
    pool_mixed = pool_mix(pool_rows, pool_gain)
    attend_cols = Q_WIDTH // N_TP
    pool_cols = POOL_WIDTH // N_TP
    summed = jnp.zeros((tokens_in.shape[0], D), jnp.float32)
    for block in range(N_TP):
        partial_sum = jnp.dot(attended[:, block * attend_cols:(block + 1) * attend_cols], attention_out_weight[block * attend_cols:(block + 1) * attend_cols], preferred_element_type=jnp.float32)
        partial_sum = partial_sum + jnp.dot(pool_mixed[:, block * pool_cols:(block + 1) * pool_cols], pool_out_weight[block * pool_cols:(block + 1) * pool_cols], preferred_element_type=jnp.float32)
        rounded = lax.optimization_barrier(partial_sum.astype(jnp.bfloat16))
        summed = summed + rounded.astype(jnp.float32)
    return summed.astype(jnp.bfloat16)
```

```python
import math

import jax
import jax.numpy as jnp
from jax import lax
from jax.sharding import PartitionSpec as P

HEAD_DIM = 64
POOL_CH = 256
POOL_GROUPS = 4
WINDOW = 128

EPS = 1e-06
SHORT_REACHES = (8, 32)


def factors(total):
    inner = max(d for d in range(1, math.isqrt(total) + 1) if total % d == 0)
    return total // inner, inner


def rotated(block, axis, inner, step_outer, step_inner):
    total = lax.axis_size(axis)
    outer = total // inner
    route = []
    for o in range(outer):
        for i in range(inner):
            target = ((o + step_outer) % outer) * inner + (i + step_inner) % inner
            route.append((o * inner + i, target))
    return lax.ppermute(block, axis, route)


def ring_blocks(block, length, rotate):
    pieces = {0: [block]}
    up = down = block
    for step in range(1, (length - 1) // 2 + 1):
        up, down = rotate(up, 1), rotate(down, -1)
        pieces[step] = [up]
        pieces[length - step] = [down]
    if length == 2:
        pieces[1] = [rotate(block, 1)]
    elif length % 2 == 0:
        half = block.shape[0] // 2
        pieces[length // 2] = [rotate(up[:half], 1), rotate(down[half:], -1)]
    return [pieces[s] for s in range(length)]


def gathering(block, axis):
    outer, inner = factors(lax.axis_size(axis))

    def far(b, d):
        return rotated(b, axis, inner, d, 0)

    def near(piece):
        return ring_blocks(piece, inner, lambda b, d: rotated(b, axis, inner, 0, d))

    arrived = {0: [near(block)]}
    up = down = block
    for step in range(1, (outer - 1) // 2 + 1):
        up, down = yield far(up, 1), far(down, -1)
        arrived[step] = [near(up)]
        arrived[outer - step] = [near(down)]
    if outer == 2:
        (up,) = yield (far(block, 1),)
        arrived[1] = [near(up)]
    elif outer % 2 == 0:
        half = block.shape[0] // 2
        top, bottom = yield far(up[:half], 1), far(down[half:], -1)
        arrived[outer // 2] = [near(top), near(bottom)]
    return [
        [piece for pieces in arrived[s] for piece in pieces[r]]
        for s in range(outer)
        for r in range(inner)
    ]


def finished(steps, started, dues=()):
    dues = list(dues)
    try:
        while True:
            if dues:
                started = lax.optimization_barrier((started, dues.pop(0)))[0]
            started = steps.send(started)
    except StopIteration as end:
        return end.value


def gathered(block, axis):
    steps = gathering(block, axis)
    return finished(steps, next(steps))


def distance_index(axis, j):
    outer, inner = factors(lax.axis_size(axis))
    me = lax.axis_index(axis)
    return (me // inner - j // inner) % outer * inner + (me % inner - j % inner) % inner


def device_at(axis, place):
    outer, inner = factors(lax.axis_size(axis))
    me = lax.axis_index(axis)
    return (me // inner - place // inner) % outer * inner + (me % inner - place % inner) % inner


def gathered_rows(block, axis):
    total = lax.axis_size(axis)
    outer, inner = total // 2, 2
    far = ring_blocks(block, outer, lambda b, d: rotated(b, axis, inner, d, 0))
    near = [[rotated(piece, axis, inner, 0, 1) for piece in pieces] for pieces in far]
    flat = [piece for pair in zip(far, near) for pieces in pair for piece in pieces]
    return flat


def scattered_sum(partial, axis):
    total = lax.axis_size(axis)
    outer, inner = total // 2, 2
    me = lax.axis_index(axis)
    rows = partial.shape[0] // total
    mine_o, mine_i = me // inner, me % inner

    def block(o, i):
        return lax.dynamic_slice_in_dim(partial, (o * inner + i) * rows, rows, 0)

    pair_sums = []
    for s in range(outer):
        o = (mine_o + s) % outer
        other = rotated(block(o, 1 - mine_i), axis, inner, 0, 1)
        pair_sums.append((o, other, s))
    result = None
    for o, other, s in pair_sums:
        both = block(o, mine_i).astype(jnp.float32) + other.astype(jnp.float32)
        if s:
            both = rotated(both.astype(jnp.bfloat16), axis, inner, s, 0).astype(jnp.float32)
        result = both if result is None else result + both
    return result.astype(jnp.bfloat16)


def passed_along(block, axis, distance):
    devices = range(lax.axis_size(axis))
    route = [(i - distance, i) for i in devices if i - distance in devices]
    return lax.ppermute(block, axis, route)


def local(
    tokens_in,
    norm_gain,
    query_weight,
    key_weight,
    value_weight,
    pool_weight,
    sink_logit,
    pool_gain,
    attention_out_weight,
    pool_out_weight,
):
    sp, tp = lax.axis_size("sp"), lax.axis_size("tp")
    k_rows = query_weight.shape[0]
    in_weights = jnp.concatenate([query_weight, key_weight, value_weight, pool_weight], axis=1)
    in_pieces = [piece for pieces in gathered(in_weights, "sp") for piece in pieces]

    widened = tokens_in.astype(jnp.float32)
    inverse = lax.rsqrt(jnp.mean(widened * widened, axis=1, keepdims=True) + EPS)
    normed = (widened * inverse * norm_gain).astype(jnp.bfloat16)
    normed = jnp.concatenate(
        [
            lax.dynamic_slice_in_dim(normed, device_at("sp", place) * k_rows, k_rows, 1)
            for place in range(sp)
        ],
        axis=1,
    )
    row_blocks = gathered_rows(normed, "tp")

    out_block = jnp.concatenate([attention_out_weight, pool_out_weight], axis=0)
    in_pieces, row_blocks, out_block = lax.optimization_barrier((in_pieces, row_blocks, out_block))
    out_steps = gathering(out_block, "sp")
    out_started = next(out_steps)

    projected = jnp.dot(
        jnp.concatenate(row_blocks, axis=0),
        jnp.concatenate(in_pieces, axis=0),
        preferred_element_type=jnp.float32,
    ).astype(jnp.bfloat16)
    t_index = lax.axis_index("tp")
    t_outer = tp // 2
    t_rows = tokens_in.shape[0]
    ordered = []
    for j in range(tp):
        place = (t_index // 2 - j // 2) % t_outer * 2 + (t_index - j) % 2
        ordered.append(lax.dynamic_slice_in_dim(projected, place * t_rows, t_rows, 0))
    projected = jnp.concatenate(ordered, axis=0)
    q_width, kv_width = query_weight.shape[1], key_weight.shape[1]
    query_rows = projected[:, :q_width]
    key_rows = projected[:, q_width : q_width + kv_width]
    value_rows = projected[:, q_width + kv_width : q_width + 2 * kv_width]
    pool_rows = projected[:, q_width + 2 * kv_width :]

    seq_len = query_rows.shape[0]
    offset = lax.axis_index("sp") * seq_len
    halo = passed_along(projected[seq_len - WINDOW :, q_width:], "sp", 1)
    halo_keys = halo[:, :kv_width]
    halo_values = halo[:, kv_width : 2 * kv_width]
    halo_pool = halo[:, 2 * kv_width :]

    pool_values = pool_rows.astype(jnp.float32)
    device_total = jnp.sum(pool_values, axis=0, keepdims=True)
    before = sum(passed_along(device_total, "sp", d) for d in range(1, sp))

    kv_local = key_rows.shape[1] // HEAD_DIM
    heads_local = query_rows.shape[1] // HEAD_DIM
    group = heads_local // kv_local
    blocks = seq_len // WINDOW
    key_ext = jnp.concatenate([halo_keys, key_rows], axis=0).reshape(
        blocks + 1, WINDOW, kv_local, HEAD_DIM
    )
    value_ext = jnp.concatenate([halo_values, value_rows], axis=0).reshape(
        blocks + 1, WINDOW, kv_local, HEAD_DIM
    )
    key_pairs = jnp.concatenate([key_ext[:-1], key_ext[1:]], axis=1)
    value_pairs = jnp.concatenate([value_ext[:-1], value_ext[1:]], axis=1)
    query_blocks = query_rows.reshape(blocks, WINDOW, kv_local, group, HEAD_DIM)
    scores = jnp.einsum(
        "nqhgd,nkhd->nhgqk", query_blocks, key_pairs, preferred_element_type=jnp.float32
    ) * HEAD_DIM ** (-0.5)
    shape_mask = (blocks, WINDOW, 2 * WINDOW)
    q_index = lax.broadcasted_iota(jnp.int32, shape_mask, 1)
    k_index = lax.broadcasted_iota(jnp.int32, shape_mask, 2)
    block_index = lax.broadcasted_iota(jnp.int32, shape_mask, 0)
    distance = q_index + WINDOW - k_index
    key_position = offset + block_index * WINDOW + k_index - WINDOW
    allowed = (distance >= 0) & (distance < WINDOW) & (key_position >= 0)
    scores = jnp.where(allowed[:, None, None], scores, -jnp.inf)
    sinks = sink_logit.reshape(1, kv_local, group, 1, 1)
    peak = jnp.maximum(jnp.max(scores, axis=-1, keepdims=True), sinks)
    expo = jnp.exp(scores - peak)
    denom = jnp.sum(expo, axis=-1, keepdims=True) + jnp.exp(sinks - peak)
    probs = (expo / denom).astype(jnp.bfloat16)
    attended = jnp.einsum(
        "nhgqk,nkhd->nqhgd", probs, value_pairs, preferred_element_type=jnp.float32
    )
    attended = attended.astype(jnp.bfloat16).reshape(seq_len, heads_local * HEAD_DIM)

    channels = pool_rows.shape[1]
    pool_ext = jnp.concatenate([halo_pool.astype(jnp.float32), pool_values], axis=0)
    running = jnp.concatenate(
        [jnp.zeros((1, channels), jnp.float32), jnp.cumsum(pool_ext, axis=0)], axis=0
    )
    group_id = lax.axis_index("tp") * channels // POOL_CH
    reach = jnp.where(
        group_id == 0, SHORT_REACHES[0], jnp.where(group_id == 1, SHORT_REACHES[1], WINDOW)
    ).astype(jnp.int32)
    upper = running[WINDOW + 1 :]
    lower = lax.dynamic_slice_in_dim(running, WINDOW + 1 - reach, seq_len, 0)
    position = offset + lax.broadcasted_iota(jnp.int32, (seq_len,), 0)
    counted = jnp.minimum(position + 1, reach).astype(jnp.float32)[:, None]
    windowed = (upper - lower) / counted
    own_sums = upper - running[WINDOW]
    cumulative = (before + own_sums) / (position + 1).astype(jnp.float32)[:, None]
    pooled = jnp.where(group_id == POOL_GROUPS - 1, cumulative, windowed)
    pool_mixed = ((pooled - pool_values) * pool_gain).astype(jnp.bfloat16)

    mixed = jnp.concatenate([attended, pool_mixed], axis=1)
    out_pieces = finished(out_steps, out_started, (projected, attended))
    out_weight = jnp.concatenate(
        [jnp.concatenate(pieces, axis=0) for pieces in out_pieces], axis=1
    )
    partial = jnp.dot(mixed, out_weight, preferred_element_type=jnp.float32).astype(jnp.bfloat16)
    summed = scattered_sum(partial, "tp")
    width = attention_out_weight.shape[1]
    return jnp.concatenate(
        [
            lax.dynamic_slice_in_dim(summed, distance_index("sp", j) * width, width, 1)
            for j in range(sp)
        ],
        axis=1,
    )


def solution(mesh):
    in_specs = (
        P(("sp", "tp"), None),
        P(),
        P("sp", "tp"),
        P("sp", "tp"),
        P("sp", "tp"),
        P("sp", "tp"),
        P("tp"),
        P("tp"),
        P("tp", "sp"),
        P("tp", "sp"),
    )
    out_specs = P(("sp", "tp"), None)
    return jax.shard_map(local, mesh=mesh, in_specs=in_specs, out_specs=out_specs, check_vma=False)
```

```python
import math

import jax
import jax.numpy as jnp
from jax import lax
from jax.experimental import pallas as pl
from jax.experimental.pallas import tpu as pltpu
from jax.sharding import PartitionSpec as P

HEAD_DIM = 64
POOL_CH = 256
POOL_GROUPS = 4
WINDOW = 128

EPS = 1e-06
SHORT_REACHES = (8, 32)


def factors(total):
    inner = max(d for d in range(1, math.isqrt(total) + 1) if total % d == 0)
    return total // inner, inner


def rotated(block, axis, inner, step_outer, step_inner):
    total = lax.axis_size(axis)
    outer = total // inner
    route = []
    for o in range(outer):
        for i in range(inner):
            target = ((o + step_outer) % outer) * inner + (i + step_inner) % inner
            route.append((o * inner + i, target))
    return lax.ppermute(block, axis, route)


def ring_blocks(block, length, rotate):
    pieces = {0: [block]}
    up = down = block
    for step in range(1, (length - 1) // 2 + 1):
        up, down = rotate(up, 1), rotate(down, -1)
        pieces[step] = [up]
        pieces[length - step] = [down]
    if length == 2:
        pieces[1] = [rotate(block, 1)]
    elif length % 2 == 0:
        half = block.shape[0] // 2
        pieces[length // 2] = [rotate(up[:half], 1), rotate(down[half:], -1)]
    return [pieces[s] for s in range(length)]


def gathering(block, axis):
    outer, inner = factors(lax.axis_size(axis))

    def far(b, d):
        return rotated(b, axis, inner, d, 0)

    def near(piece):
        return ring_blocks(piece, inner, lambda b, d: rotated(b, axis, inner, 0, d))

    arrived = {0: [near(block)]}
    up = down = block
    for step in range(1, (outer - 1) // 2 + 1):
        up, down = yield far(up, 1), far(down, -1)
        arrived[step] = [near(up)]
        arrived[outer - step] = [near(down)]
    if outer == 2:
        (up,) = yield (far(block, 1),)
        arrived[1] = [near(up)]
    elif outer % 2 == 0:
        half = block.shape[0] // 2
        top, bottom = yield far(up[:half], 1), far(down[half:], -1)
        arrived[outer // 2] = [near(top), near(bottom)]
    return [
        [piece for pieces in arrived[s] for piece in pieces[r]]
        for s in range(outer)
        for r in range(inner)
    ]


def finished(steps, started, dues=()):
    dues = list(dues)
    try:
        while True:
            if dues:
                started = lax.optimization_barrier((started, dues.pop(0)))[0]
            started = steps.send(started)
    except StopIteration as end:
        return end.value


def gathered(block, axis):
    steps = gathering(block, axis)
    return finished(steps, next(steps))


def device_at(axis, place):
    outer, inner = factors(lax.axis_size(axis))
    me = lax.axis_index(axis)
    return (me // inner - place // inner) % outer * inner + (me % inner - place % inner) % inner


def gathered_rows(block, axis):
    total = lax.axis_size(axis)
    outer, inner = total // 2, 2
    far = ring_blocks(block, outer, lambda b, d: rotated(b, axis, inner, d, 0))
    near = [[rotated(piece, axis, inner, 0, 1) for piece in pieces] for pieces in far]
    return far, near


def scattered_sum(partial, axis):
    total = lax.axis_size(axis)
    outer, inner = total // 2, 2
    me = lax.axis_index(axis)
    rows = partial.shape[0] // total
    mine_o, mine_i = me // inner, me % inner

    def block(o, i):
        return lax.dynamic_slice_in_dim(partial, (o * inner + i) * rows, rows, 0)

    pair_sums = []
    for s in range(outer):
        o = (mine_o + s) % outer
        other = rotated(block(o, 1 - mine_i), axis, inner, 0, 1)
        pair_sums.append((o, other, s))
    result = None
    for o, other, s in pair_sums:
        both = block(o, mine_i).astype(jnp.float32) + other.astype(jnp.float32)
        if s:
            both = rotated(both.astype(jnp.bfloat16), axis, inner, s, 0).astype(jnp.float32)
        result = both if result is None else result + both
    return result.astype(jnp.bfloat16)


def passed_along(block, axis, distance):
    devices = range(lax.axis_size(axis))
    route = [(i - distance, i) for i in devices if i - distance in devices]
    return lax.ppermute(block, axis, route)


VMEM = pl.BlockSpec(memory_space=pltpu.VMEM)
SMEM = pl.BlockSpec(memory_space=pltpu.SMEM)


def project(row_pieces, row_starts, weight_pieces, weight_starts):
    n_rows, n_weights = len(row_pieces), len(weight_pieces)
    seq_len = sum(piece.shape[0] for piece in row_pieces)
    width = weight_pieces[0].shape[1]

    def kernel(row_starts_ref, weight_starts_ref, *refs):
        rows, weights, out = refs[:n_rows], refs[n_rows:-1], refs[-1]
        total = None
        for w in range(n_weights):
            depth = weights[w].shape[0]
            start = pl.multiple_of(weight_starts_ref[w], 128)
            left = jnp.concatenate([row[:, pl.ds(start, depth)] for row in rows], axis=0)
            product = jnp.dot(left, weights[w][...], preferred_element_type=jnp.float32)
            total = product if total is None else total + product
        rounded = total.astype(jnp.bfloat16)
        at = 0
        for r in range(n_rows):
            count = rows[r].shape[0]
            start = pl.multiple_of(row_starts_ref[r], 16)
            out[pl.ds(start, count), :] = rounded[at : at + count]
            at += count

    return pl.pallas_call(
        kernel,
        out_shape=jax.ShapeDtypeStruct((seq_len, width), jnp.bfloat16),
        in_specs=[SMEM, SMEM] + [VMEM] * (n_rows + n_weights),
        out_specs=VMEM,
        name="project",
    )(row_starts, weight_starts, *row_pieces, *weight_pieces)


def attend(projected, halo, sink_logit, offset, q_width, kv_width):
    seq_len = projected.shape[0]
    heads, kv_heads = q_width // HEAD_DIM, kv_width // HEAD_DIM
    group = heads // kv_heads

    def kernel(offset_ref, sink_ref, projected_ref, halo_ref, out_ref, ext_ref):
        ext_ref[:WINDOW] = halo_ref[:, : 2 * kv_width]
        ext_ref[WINDOW:] = projected_ref[:, q_width : q_width + 2 * kv_width]
        q_index = lax.broadcasted_iota(jnp.int32, (WINDOW, 2 * WINDOW), 0)
        k_index = lax.broadcasted_iota(jnp.int32, (WINDOW, 2 * WINDOW), 1)
        distance = q_index + WINDOW - k_index
        inside = (distance >= 0) & (distance < WINDOW)
        for n in range(seq_len // WINDOW):
            allowed = inside
            if n == 0:
                allowed = inside & (offset_ref[0] + k_index - WINDOW >= 0)
            query = projected_ref[n * WINDOW : (n + 1) * WINDOW, :q_width]
            ext = ext_ref[n * WINDOW : (n + 2) * WINDOW, :]
            outs = []
            for h in range(heads):
                k_at = h // group * HEAD_DIM
                scores = lax.dot_general(
                    query[:, h * HEAD_DIM : (h + 1) * HEAD_DIM],
                    ext[:, k_at : k_at + HEAD_DIM],
                    (((1,), (1,)), ((), ())),
                    preferred_element_type=jnp.float32,
                ) * HEAD_DIM ** (-0.5)
                scores = jnp.where(allowed, scores, -jnp.inf)
                sink = sink_ref[h]
                peak = jnp.maximum(jnp.max(scores, axis=1, keepdims=True), sink)
                expo = jnp.exp(scores - peak)
                denom = jnp.sum(expo, axis=1, keepdims=True) + jnp.exp(sink - peak)
                probs = (expo / denom).astype(jnp.bfloat16)
                values = ext[:, kv_width + k_at : kv_width + k_at + HEAD_DIM]
                outs.append(jnp.dot(probs, values, preferred_element_type=jnp.float32))
            out_ref[n * WINDOW : (n + 1) * WINDOW, :] = jnp.concatenate(outs, axis=1).astype(
                jnp.bfloat16
            )

    return pl.pallas_call(
        kernel,
        out_shape=jax.ShapeDtypeStruct((seq_len, q_width), jnp.bfloat16),
        in_specs=[SMEM, SMEM, VMEM, VMEM],
        out_specs=VMEM,
        scratch_shapes=[pltpu.VMEM((seq_len + WINDOW, 2 * kv_width), jnp.bfloat16)],
        name="attend",
    )(offset[None], sink_logit, projected, halo)


def pool(projected, halo, before, pool_gain, offset, group_id):
    seq_len, channels = projected.shape[0], pool_gain.shape[0]
    first, halo_first = projected.shape[1] - channels, halo.shape[1] - channels
    short, middle = SHORT_REACHES

    def kernel(scalars_ref, projected_ref, halo_ref, before_ref, gain_ref, out_ref):
        start, group = scalars_ref[0], scalars_ref[1]
        whole = group == POOL_GROUPS - 1
        reach = jnp.where(group == 0, short, jnp.where(group == 1, middle, WINDOW))
        q_index = lax.broadcasted_iota(jnp.int32, (WINDOW, 2 * WINDOW), 0)
        k_index = lax.broadcasted_iota(jnp.int32, (WINDOW, 2 * WINDOW), 1)
        distance = q_index + WINDOW - k_index
        limit = jnp.where(whole, q_index + 1, reach)
        band = jnp.where((distance >= 0) & (distance < limit), 1.0, 0.0).astype(jnp.bfloat16)
        carried = before_ref[...]
        keep = jnp.where(whole, 1.0, 0.0)
        for n in range(seq_len // WINDOW):
            rows = projected_ref[n * WINDOW : (n + 1) * WINDOW, first:]
            if n:
                earlier = projected_ref[(n - 1) * WINDOW : n * WINDOW, first:]
            else:
                earlier = halo_ref[:, halo_first:]
            sums = jnp.dot(
                band,
                jnp.concatenate([earlier, rows], axis=0),
                preferred_element_type=jnp.float32,
            )
            values = rows.astype(jnp.float32)
            position = start + n * WINDOW + lax.broadcasted_iota(jnp.int32, (WINDOW, 1), 0)
            count = jnp.where(whole, position + 1, jnp.minimum(position + 1, reach))
            pooled = (sums + keep * carried) / count.astype(jnp.float32)
            carried = carried + jnp.sum(values, axis=0, keepdims=True)
            out_ref[n * WINDOW : (n + 1) * WINDOW, :] = (
                (pooled - values) * gain_ref[...]
            ).astype(jnp.bfloat16)

    return pl.pallas_call(
        kernel,
        out_shape=jax.ShapeDtypeStruct((seq_len, channels), jnp.bfloat16),
        in_specs=[SMEM, VMEM, VMEM, VMEM, VMEM],
        out_specs=VMEM,
        name="pool",
    )(jnp.stack([offset, group_id]), projected, halo, before, pool_gain[None, :])


def multiply_out(attended, pool_mixed, out_blocks, starts):
    counts = [len(pieces) for pieces in out_blocks]
    flat = [piece for pieces in out_blocks for piece in pieces]
    width = flat[0].shape[1]

    def kernel(starts_ref, attended_ref, pool_ref, *refs):
        weights, out = refs[:-1], refs[-1]
        left = jnp.concatenate([attended_ref[...], pool_ref[...]], axis=1)
        at = 0
        for b, count in enumerate(counts):
            pieces = [ref[...] for ref in weights[at : at + count]]
            at += count
            weight = pieces[0] if count == 1 else jnp.concatenate(pieces, axis=0)
            product = jnp.dot(left, weight, preferred_element_type=jnp.float32)
            start = pl.multiple_of(starts_ref[b], 128)
            out[:, pl.ds(start, width)] = product.astype(jnp.bfloat16)

    return pl.pallas_call(
        kernel,
        out_shape=jax.ShapeDtypeStruct(
            (attended.shape[0], width * len(counts)), jnp.bfloat16
        ),
        in_specs=[SMEM] + [VMEM] * (2 + len(flat)),
        out_specs=VMEM,
        name="multiply_out",
    )(starts, attended, pool_mixed, *flat)


def summed_before(own, axis):
    total, distance = own, 1
    while distance < lax.axis_size(axis):
        total = total + passed_along(total, axis, distance)
        distance *= 2
    return total - own


def local(
    tokens_in,
    norm_gain,
    query_weight,
    key_weight,
    value_weight,
    pool_weight,
    sink_logit,
    pool_gain,
    attention_out_weight,
    pool_out_weight,
):
    sp, tp = lax.axis_size("sp"), lax.axis_size("tp")
    k_rows = query_weight.shape[0]
    in_weights = jnp.concatenate([query_weight, key_weight, value_weight, pool_weight], axis=1)
    in_blocks = gathered(in_weights, "sp")
    in_pieces, in_starts = [], []
    for place, pieces in enumerate(in_blocks):
        start = device_at("sp", place) * k_rows
        for piece in pieces:
            in_pieces.append(piece)
            in_starts.append(start)
            start = start + piece.shape[0]

    widened = tokens_in.astype(jnp.float32)
    inverse = lax.rsqrt(jnp.mean(widened * widened, axis=1, keepdims=True) + EPS)
    normed = (widened * inverse * norm_gain).astype(jnp.bfloat16)
    far, near = gathered_rows(normed, "tp")
    t_index, t_rows = lax.axis_index("tp"), tokens_in.shape[0]
    row_blocks, row_starts = [], []
    for s in range(tp // 2):
        for inner, pieces in enumerate((far[s], near[s])):
            start = ((t_index // 2 - s) % (tp // 2) * 2 + (t_index + inner) % 2) * t_rows
            for piece in pieces:
                row_blocks.append(piece)
                row_starts.append(start)
                start = start + piece.shape[0]

    out_block = jnp.concatenate([attention_out_weight, pool_out_weight], axis=0)
    in_pieces, row_blocks, out_block = lax.optimization_barrier((in_pieces, row_blocks, out_block))
    out_steps = gathering(out_block, "sp")
    out_started = next(out_steps)

    projected = project(row_blocks, jnp.stack(row_starts), in_pieces, jnp.stack(in_starts))
    q_width, kv_width = query_weight.shape[1], key_weight.shape[1]
    channels = pool_weight.shape[1]
    seq_len = projected.shape[0]
    offset = lax.axis_index("sp") * seq_len
    halo = passed_along(projected[seq_len - WINDOW :, q_width:], "sp", 1)
    device_total = jnp.sum(
        projected[:, q_width + 2 * kv_width :].astype(jnp.float32), axis=0, keepdims=True
    )
    before = summed_before(device_total, "sp")
    attended = attend(projected, halo, sink_logit, offset, q_width, kv_width)
    group_id = t_index * channels // POOL_CH
    pool_mixed = pool(projected, halo, before, pool_gain, offset, group_id)

    out_blocks = finished(out_steps, out_started, (projected, attended))
    width = attention_out_weight.shape[1]
    starts = jnp.stack([device_at("sp", place) * width for place in range(sp)])
    partial = multiply_out(attended, pool_mixed, out_blocks, starts)
    return scattered_sum(partial, "tp")


def solution(mesh):
    in_specs = (
        P(("sp", "tp"), None),
        P(),
        P("sp", "tp"),
        P("sp", "tp"),
        P("sp", "tp"),
        P("sp", "tp"),
        P("tp"),
        P("tp"),
        P("tp", "sp"),
        P("tp", "sp"),
    )
    out_specs = P(("sp", "tp"), None)
    return jax.shard_map(local, mesh=mesh, in_specs=in_specs, out_specs=out_specs, check_vma=False)
```
